32 devices in a mesh: ep: 8 (over z, y), tp: 4 (over x, core).
Axes of the slice: x: 2, y: 2, z: 4, core: 2. Of those that a mesh axis runs over, the one named last changes fastest.
Arguments:
- queries: bfloat16 [8192, 1024], P('ep', 'tp'), may hold values from -6 to 6
- head_keys: bfloat16 [8192, 256], P('ep', 'tp'), may hold values from -6 to 6
- head_values: bfloat16 [8192, 256], P('ep', 'tp'), may hold values from -6 to 6
- sink_logits: float32 [16], P('tp'), may hold values from -2 to 5
- out_weight: bfloat16 [1024, 2048], P('tp'), may hold values from -1.5 to 1.5
- moe_input: bfloat16 [4096, 2048], P(('ep', 'tp')), may hold values from -6 to 6
- norm_gain: float32 [2048], replicated, may hold values from 0.1 to 1.9
- routes: int32 [4096, 4], P(('ep', 'tp')), may hold values from 0 to 7, all different within a row; in each aligned block of 128 rows (0 to 127, 128 to 255, ...) at most 128 rows name the same one
- route_weight: float32 [4096, 4], P(('ep', 'tp')), may hold values from 0.05 to 1
- gate_weight: bfloat16 [8, 2048, 512], P('ep'), may hold values from -2 to 2
- up_weight: bfloat16 [8, 2048, 512], P('ep'), may hold values from -2 to 2
- down_weight: bfloat16 [8, 512, 2048], P('ep'), may hold values from -0.25 to 0.25
Outputs:
- attention_out: bfloat16 [8192, 2048], P(('ep', 'tp'))
- routed_out: bfloat16 [4096, 2048], P(('ep', 'tp'))
The draws below stay inside these ranges and needn't reach their ends.
Inputs may be any that keep to these rules, and one draw needn't show every extreme that they name: `routes`: within the rows of one device (aligned blocks of 128 rows), each expert is named by at most 128 rows, and in every draw some expert by exactly 128; a row names 4 different experts.
All inputs are finite; a program needn't handle non-finite values.
Results may differ from the reference program's by a relative error of at most 0.0078.
Values may be sent and summed in bfloat16 or wider, within the bound.
A program may use at most 128 MiB of HBM per device.

```python
import math
import jax
import jax.numpy as jnp
import numpy as np
from jax import lax

D = 2048
HEADS = 16
KV_HEADS = 4
HEAD_DIM = 64
WINDOW = 128
SEQS = 1
FF = 512
TOPK = 4
TOK_M = 128
EXPERTS = 8
CAP = 128
TOKENS_A = 8192
TOKENS_M = 4096


def draw_queries(key, part):
    per_group = HEADS // KV_HEADS
    normal = jax.random.normal(jax.random.fold_in(key, 1), (TOKENS_A, KV_HEADS, per_group, HEAD_DIM), jnp.float32)
    normal = jnp.clip(normal, -6.0, 6.0)
    return normal.reshape(TOKENS_A, HEADS * HEAD_DIM).astype(jnp.bfloat16)


def draw_head_keys(key, part):
    normal = jax.random.normal(jax.random.fold_in(key, 2), (TOKENS_A, KV_HEADS, 1, HEAD_DIM), jnp.float32)
    normal = jnp.clip(normal, -6.0, 6.0)
    return normal.reshape(TOKENS_A, KV_HEADS * HEAD_DIM).astype(jnp.bfloat16)


def expert_matrix(key, salt):
    normal = jax.random.normal(jax.random.fold_in(key, salt), (EXPERTS, D, FF), jnp.float32)
    normal = jnp.clip(normal, -6.0, 6.0) * D ** (-0.5)
    return jnp.clip(normal, -2.0, 2.0).astype(jnp.bfloat16)


def draw_gate_weight(key, part):
    return expert_matrix(key, 11)


def draw_up_weight(key, part):
    return expert_matrix(key, 13)


def block_scale(stream_key, shape, pieces, low, top_value):
    factor_of, own = 1.0, jax.random.fold_in(stream_key, 6)
    for position, parts in pieces:
        draws = jnp.exp(jax.random.uniform(jax.random.fold_in(own, position), (parts,), jnp.float32, low / len(pieces), top_value / len(pieces)))
        factor_of = factor_of * jnp.repeat(draws, shape[position] // parts).reshape([-1 if axis == position else 1 for axis in range(len(shape))])
    return factor_of


def deal_out(key, own, number, rows, number_of, top, limit, lean):
    sequence = jax.random.permutation(key, number_of)
    crowded, ordinary = shares(number_of, rows * top, limit, lean, True), shares(number_of, rows * top, limit, lean, False)
    places = jnp.arange(number_of)

    def named(tallies, turn):
        used = int((tallies > 0).sum())
        fixed = max(1, used // 4)
        passed = fixed + (places - fixed + turn * (used - fixed)) % max(1, number_of - fixed)
        return jnp.zeros((number_of,), jnp.int32).at[sequence[jnp.where(places < fixed, places, passed)]].set(jnp.asarray(tallies, jnp.int32))

    tallies = jnp.where(number % 4 == 0, named(crowded, number // 4), named(ordinary, number - number // 4 - 1))
    mixed = jax.random.permutation(jax.random.fold_in(own, 3), number_of)
    giver, sink = mixed[0:number_of // 2 * 2:2], mixed[1:number_of // 2 * 2:2]
    margin = jnp.minimum(tallies[giver] - 1, limit - tallies[sink]) // 2
    margin = jnp.where((giver == sequence[0]) | (sink == sequence[0]) | (tallies[sink] == 0), 0, jnp.maximum(margin, 0))
    passed = jax.random.randint(jax.random.fold_in(own, 4), (number_of // 2,), 0, 1 << 20) % (margin + 1)
    tallies = tallies.at[giver].add(-passed).at[sink].add(passed)
    labels = jnp.searchsorted(jnp.cumsum(tallies), jnp.arange(rows * top), side="right").astype(jnp.int32)
    listing = labels.reshape(top, rows).T
    listing = listing[jax.random.permutation(jax.random.fold_in(own, 1), rows)]
    turn = jax.random.randint(jax.random.fold_in(own, 2), (rows, 1), 0, top)
    return jnp.take_along_axis(listing, (jnp.arange(top)[None, :] + turn) % top, axis=1)


def shares(number_of, total, most, skew, full):
    portions = [(1 << 20) // math.isqrt(standing ** skew) + 1 for standing in range(1, number_of + 1)]
    largest = most if full else min(most, max(-(-total // number_of), total * portions[0] // sum(portions)))
    least = 1 if total - largest >= number_of - 1 else 0
    given, rest = [largest] + [least] * (number_of - 1), total - largest - least * (number_of - 1)
    while rest > 0:
        candidates = [i for i in range(1, number_of) if given[i] < largest] or [i for i in range(1, number_of) if given[i] < most]
        mass, remaining = sum([portions[i] for i in candidates]), rest
        for i in candidates:
            addition = min(most - given[i], max(1, remaining * portions[i] // mass), rest)
            given[i] = given[i] + addition
            rest = rest - addition
    return np.array(given)


def gaussian(key, shape, spread, reach, split=(), kind=jnp.bfloat16):
    drawn = jax.random.normal(key, shape, jnp.float32) * spread
    if len(split) > 0:
        drawn = block_scale(key, shape, split, -0.22, 0.18) * drawn
    return jnp.clip(drawn, min=-reach, max=reach).astype(kind)


def setup_inputs(seed: int = 0) -> dict:
    streams_of = jax.random.split(jax.random.key(seed), 13)
    queries = draw_queries(jax.random.fold_in(streams_of[12], 71), 0)
    head_keys = draw_head_keys(jax.random.fold_in(streams_of[12], 71), 0)
    head_values = gaussian(streams_of[2], (TOKENS_A, KV_HEADS * HEAD_DIM), 1.0, 6.0, ((0, 8), (1, 4)))
    sink_logits = jnp.clip(-2.0 + 7.0 * jax.random.uniform(streams_of[3], (HEADS,), jnp.float32) ** block_scale(streams_of[3], (HEADS,), ((0, 4),), -0.2, 0.2), -2.0, 5.0)
    out_weight = gaussian(streams_of[4], (HEADS * HEAD_DIM, D), 0.25, 1.5, ((0, 4),))
    moe_input = gaussian(streams_of[5], (TOKENS_M, D), 1.0, 6.0, ((0, 32),))
    norm_gain = jnp.clip(1.0 + 0.18 * jax.random.normal(streams_of[6], (D,), jnp.float32), 0.1, 1.9)
    routes_keys = jax.random.split(jax.random.fold_in(streams_of[7], 1), TOKENS_M // TOK_M)
    routes_turns = jax.random.permutation(jax.random.fold_in(streams_of[7], 3), TOKENS_M // TOK_M)
    routes = jax.vmap(lambda own, number: deal_out(jax.random.fold_in(streams_of[7], 2), own, number, TOK_M, EXPERTS, TOPK, CAP, 1))(routes_keys, routes_turns).reshape((TOKENS_M, TOPK))
    route_weight = jnp.clip(jnp.exp(math.log(1.0) - 2.9957323 * jax.random.uniform(streams_of[8], (TOKENS_M, TOPK), jnp.float32) ** block_scale(streams_of[8], (TOKENS_M, TOPK), ((0, 32),), -0.2, 0.2)), 0.05, 1.0)
    gate_weight = draw_gate_weight(jax.random.fold_in(streams_of[12], 71), 0)
    up_weight = draw_up_weight(jax.random.fold_in(streams_of[12], 71), 0)
    down_weight = gaussian(streams_of[11], (EXPERTS, FF, D), FF ** -0.5, 0.25, ((0, 8),))
    return dict(queries=queries, head_keys=head_keys, head_values=head_values, sink_logits=sink_logits, out_weight=out_weight, moe_input=moe_input, norm_gain=norm_gain, routes=routes, route_weight=route_weight, gate_weight=gate_weight, up_weight=up_weight, down_weight=down_weight)


EPSILON = 1e-05
NEGATIVE = -1e+30

def clamped_unit(gate_pre, up_pre):
    gate_cut = jnp.minimum(gate_pre, 7.0)
    up_cut = jnp.clip(up_pre, -7.0, 7.0)
    return gate_cut * jax.nn.sigmoid(1.702 * gate_cut) * (up_cut + 1.0)

def window_attention(queries, head_keys, head_values, sink_logits, out_weight):
    total = queries.shape[0]
    per_group = HEADS // KV_HEADS
    seq_len = TOKENS_A // SEQS
    padding = jnp.zeros((WINDOW, KV_HEADS * HEAD_DIM), head_keys.dtype)
    padded_keys = jnp.concatenate([padding, head_keys], axis=0)
    padded_values = jnp.concatenate([padding, head_values], axis=0)
    sinks = sink_logits.astype(jnp.float32).reshape(KV_HEADS, per_group, 1, 1)

    def one_block(index):
        first = (index * WINDOW).astype(jnp.int32)
        block_q = lax.dynamic_slice_in_dim(queries, first, WINDOW, 0)
        block_q = block_q.reshape(WINDOW, KV_HEADS, per_group, HEAD_DIM).astype(jnp.float32)
        block_k = lax.dynamic_slice_in_dim(padded_keys, first, 2 * WINDOW, 0)
        block_k = block_k.reshape(2 * WINDOW, KV_HEADS, HEAD_DIM).astype(jnp.float32)
        block_v = lax.dynamic_slice_in_dim(padded_values, first, 2 * WINDOW, 0)
        block_v = block_v.reshape(2 * WINDOW, KV_HEADS, HEAD_DIM).astype(jnp.float32)
        scores = jnp.einsum('qkgd,skd->kgqs', block_q, block_k) * HEAD_DIM ** (-0.5)
        query_pos = first + jnp.arange(WINDOW, dtype=jnp.int32)
        key_pos = first - WINDOW + jnp.arange(2 * WINDOW, dtype=jnp.int32)
        distance = query_pos[:, None] - key_pos[None, :]
        starts = query_pos // seq_len * seq_len
        valid = (distance >= 0) & (distance < WINDOW) & (key_pos[None, :] >= starts[:, None])
        scores = jnp.where(valid[None, None], scores, NEGATIVE)
        maxima = jnp.maximum(lax.optimization_barrier(jnp.max(scores, axis=-1, keepdims=True)), sinks)
        powers = jnp.exp(scores - maxima)
        weights = powers / (lax.optimization_barrier(jnp.sum(powers, axis=-1, keepdims=True)) + jnp.exp(sinks - maxima))
        weights = weights.astype(jnp.bfloat16)
        heads = jnp.einsum('kgqs,skd->qkgd', weights.astype(jnp.float32), block_v)
        return heads.astype(jnp.bfloat16).reshape(WINDOW, HEADS * HEAD_DIM)
    heads_out = lax.map(one_block, jnp.arange(total // WINDOW, dtype=jnp.int32))
    heads_out = heads_out.reshape(total, HEADS * HEAD_DIM)
    return jnp.dot(heads_out, out_weight, preferred_element_type=jnp.float32).astype(jnp.bfloat16)

def routed_experts(moe_input, norm_gain, routes, route_weight, gate_weight, up_weight, down_weight):
    token_count = moe_input.shape[0]
    values32 = moe_input.astype(jnp.float32)
    scale = lax.rsqrt(lax.optimization_barrier(jnp.mean(values32 * values32, axis=-1, keepdims=True)) + EPSILON)
    normed = (values32 * scale * norm_gain.astype(jnp.float32)).astype(jnp.bfloat16)
    assigned = token_count * TOPK
    group_rows = 256
    flat_routes = routes.reshape(assigned).astype(jnp.int32)
    token_of = (jnp.arange(assigned, dtype=jnp.int32) // TOPK).astype(jnp.int32)
    order = jnp.argsort(flat_routes, stable=True).astype(jnp.int32)
    sorted_routes = flat_routes[order]
    counts = lax.optimization_barrier(jnp.sum((flat_routes[:, None] == jnp.arange(EXPERTS, dtype=jnp.int32)[None, :]).astype(jnp.int32), axis=0)).astype(jnp.int32)
    padded = ((counts + group_rows - 1) // group_rows * group_rows).astype(jnp.int32)
    end_pad = jnp.cumsum(padded).astype(jnp.int32)
    start_pad = (end_pad - padded).astype(jnp.int32)
    start_raw = (jnp.cumsum(counts) - counts).astype(jnp.int32)
    dest = (start_pad[sorted_routes] + jnp.arange(assigned, dtype=jnp.int32) - start_raw[sorted_routes]).astype(jnp.int32)
    group_count = -(-assigned // group_rows) + EXPERTS
    slot_total = group_count * group_rows
    row_token = jnp.zeros((slot_total,), jnp.int32).at[dest].set(token_of[order])
    row_weight = jnp.zeros((slot_total,), jnp.float32).at[dest].set(route_weight.reshape(assigned).astype(jnp.float32)[order])
    group_expert = jnp.searchsorted(end_pad, jnp.arange(group_count, dtype=jnp.int32) * group_rows, side='right')
    group_expert = jnp.minimum(group_expert, EXPERTS - 1).astype(jnp.int32)

    def add_group(total, inputs):
        expert, tokens, weights = inputs
        rows_in = normed[tokens]
        gate_pre = jnp.dot(rows_in, gate_weight[expert], preferred_element_type=jnp.float32)
        up_pre = jnp.dot(rows_in, up_weight[expert], preferred_element_type=jnp.float32)
        act = clamped_unit(gate_pre, up_pre).astype(jnp.bfloat16)
        result = jnp.dot(act, down_weight[expert], preferred_element_type=jnp.float32).astype(jnp.bfloat16)
        return (total.at[tokens].add(result.astype(jnp.float32) * weights[:, None]), None)
    initial = jnp.zeros((token_count, D), jnp.float32)
    total, _ = lax.scan(add_group, initial, (group_expert, row_token.reshape(group_count, group_rows), row_weight.reshape(group_count, group_rows)))
    return total.astype(jnp.bfloat16)

def reference(queries, head_keys, head_values, sink_logits, out_weight, moe_input, norm_gain, routes, route_weight, gate_weight, up_weight, down_weight):
    attention_out = window_attention(queries, head_keys, head_values, sink_logits, out_weight)
    routed_out = routed_experts(moe_input, norm_gain, routes, route_weight, gate_weight, up_weight, down_weight)
    return (attention_out, routed_out)
```

```python
import jax
import jax.numpy as jnp
from jax import lax
from jax.sharding import PartitionSpec as P

HEAD_DIM = 64
WINDOW = 128
SEQS = 1


EPSILON = 1e-05
NEGATIVE = -1e30


def passed_along(value, axis, steps):
    count = lax.axis_size(axis)
    first, last = (max(0, -steps), min(count, count - steps))
    return lax.ppermute(value, axis, [(source, source + steps) for source in range(first, last)])


def clamped_unit(gate_pre, up_pre):
    gate_cut = jnp.minimum(gate_pre, 7.0)
    up_cut = jnp.clip(up_pre, -7.0, 7.0)
    return gate_cut * jax.nn.sigmoid(1.702 * gate_cut) * (up_cut + 1.0)


def attend(queries, head_keys, head_values, sink_logits, out_weight):
    tok_rows = queries.shape[0]
    local_heads = sink_logits.shape[0]
    local_kv = head_keys.shape[1] // HEAD_DIM
    per_group = local_heads // local_kv
    block_count = tok_rows // WINDOW
    key_width = local_kv * HEAD_DIM
    kv_rows = jnp.concatenate([head_keys, head_values], axis=1)
    earlier = passed_along(kv_rows[tok_rows - WINDOW :], "ep", 1)
    extended = jnp.concatenate([earlier, kv_rows], axis=0)
    banded = jnp.concatenate(
        [
            extended[:tok_rows].reshape(block_count, WINDOW, 2 * key_width),
            kv_rows.reshape(block_count, WINDOW, 2 * key_width),
        ],
        axis=1,
    )
    band_keys = banded[:, :, :key_width].reshape(block_count, 2 * WINDOW, local_kv, HEAD_DIM)
    band_values = banded[:, :, key_width:].reshape(block_count, 2 * WINDOW, local_kv, HEAD_DIM)
    blocked = queries.reshape(block_count, WINDOW, local_kv, per_group, HEAD_DIM)
    scores = jnp.einsum(
        "nqkgd,nskd->nkgqs", blocked, band_keys, preferred_element_type=jnp.float32
    ) * HEAD_DIM ** (-0.5)
    offset = lax.axis_index("ep") * tok_rows
    seq_len = tok_rows * lax.axis_size("ep") // SEQS
    query_pos = offset + jnp.arange(tok_rows, dtype=jnp.int32).reshape(block_count, WINDOW)
    key_pos = (
        offset
        - WINDOW
        + (jnp.arange(block_count, dtype=jnp.int32) * WINDOW)[:, None]
        + jnp.arange(2 * WINDOW, dtype=jnp.int32)[None, :]
    )
    distance = query_pos[:, :, None] - key_pos[:, None, :]
    starts = query_pos // seq_len * seq_len
    valid = (distance >= 0) & (distance < WINDOW) & (key_pos[:, None, :] >= starts[:, :, None])
    scores = jnp.where(valid[:, None, None], scores, NEGATIVE)
    sinks = sink_logits.reshape(local_kv, per_group, 1, 1)
    maxima = jnp.maximum(jnp.max(scores, axis=-1, keepdims=True), sinks)
    powers = jnp.exp(scores - maxima)
    weights = (powers / (jnp.sum(powers, axis=-1, keepdims=True) + jnp.exp(sinks - maxima))).astype(
        jnp.bfloat16
    )
    heads_out = jnp.einsum(
        "nkgqs,nskd->nqkgd", weights, band_values, preferred_element_type=jnp.float32
    )
    heads_out = heads_out.astype(jnp.bfloat16).reshape(tok_rows, local_heads * HEAD_DIM)
    summed = lax.psum_scatter(
        jnp.dot(heads_out, out_weight, preferred_element_type=jnp.float32),
        "tp",
        scatter_dimension=0,
        tiled=True,
    )
    return summed.astype(jnp.bfloat16)


def experts_part(moe_input, norm_gain, routes, route_weight, gate_weight, up_weight, down_weight):
    tok_rows, model_width = moe_input.shape
    choice_count = routes.shape[1]
    targets = lax.axis_size("ep")
    capacity = 2 * choice_count * tok_rows // targets
    values32 = moe_input.astype(jnp.float32)
    scale = lax.rsqrt(jnp.mean(values32 * values32, axis=-1, keepdims=True) + EPSILON)
    normed = (values32 * scale * norm_gain).astype(jnp.bfloat16)
    if capacity >= tok_rows:
        experts = jnp.arange(targets, dtype=jnp.int32)
        named = routes[:, :, None] == experts[None, None, :]
        shares = jnp.sum(jnp.where(named, route_weight[:, :, None], 0.0), axis=1)
        everyone = lax.all_gather(normed, "ep", axis=0, tiled=True)
        mine = lax.all_to_all(shares.T[:, None], "ep", split_axis=0, concat_axis=0, tiled=True)
        gate_pre = jnp.dot(everyone, gate_weight[0], preferred_element_type=jnp.float32)
        up_pre = jnp.dot(everyone, up_weight[0], preferred_element_type=jnp.float32)
        act = clamped_unit(gate_pre, up_pre).astype(jnp.bfloat16)
        result = jnp.dot(act, down_weight[0], preferred_element_type=jnp.float32)
        part = result.astype(jnp.bfloat16).astype(jnp.float32) * mine.reshape(-1, 1)
        return lax.psum_scatter(
            part.astype(jnp.bfloat16), "ep", scatter_dimension=0, tiled=True
        )
    flat_routes = routes.reshape(-1)
    onehot = (flat_routes[:, None] == jnp.arange(targets, dtype=jnp.int32)[None, :]).astype(
        jnp.int32
    )
    earlier_count = jnp.sum((jnp.cumsum(onehot, axis=0) - onehot) * onehot, axis=1)
    slot_index = flat_routes * capacity + earlier_count
    copies = jnp.repeat(normed, choice_count, axis=0)
    outgoing = jnp.zeros((targets * capacity, model_width), jnp.bfloat16).at[slot_index].set(copies)
    outgoing = outgoing.reshape(targets, capacity, model_width)
    arrived = lax.all_to_all(outgoing, "ep", split_axis=0, concat_axis=0, tiled=True)
    flat_rows = arrived.reshape(-1, model_width)
    gate_pre = jnp.dot(flat_rows, gate_weight[0], preferred_element_type=jnp.float32)
    up_pre = jnp.dot(flat_rows, up_weight[0], preferred_element_type=jnp.float32)
    act = clamped_unit(gate_pre, up_pre).astype(jnp.bfloat16)
    result = jnp.dot(act, down_weight[0], preferred_element_type=jnp.float32).astype(jnp.bfloat16)
    came_back = lax.all_to_all(
        result.reshape(arrived.shape), "ep", split_axis=0, concat_axis=0, tiled=True
    )
    picked = came_back.reshape(targets * capacity, model_width)[slot_index]
    weighted = (
        picked.astype(jnp.float32).reshape(tok_rows, choice_count, model_width)
        * route_weight[:, :, None]
    )
    return jnp.sum(weighted, axis=1).astype(jnp.bfloat16)


def on_device(
    queries,
    head_keys,
    head_values,
    sink_logits,
    out_weight,
    moe_input,
    norm_gain,
    routes,
    route_weight,
    gate_weight,
    up_weight,
    down_weight,
):
    attention_out = attend(queries, head_keys, head_values, sink_logits, out_weight)
    routed_out = experts_part(
        moe_input, norm_gain, routes, route_weight, gate_weight, up_weight, down_weight
    )
    return (attention_out, routed_out)


def solution(mesh):
    placed = (
        P("ep", "tp"),
        P("ep", "tp"),
        P("ep", "tp"),
        P("tp"),
        P("tp", None),
        P(("ep", "tp"), None),
        P(),
        P(("ep", "tp"), None),
        P(("ep", "tp"), None),
        P("ep", None, None),
        P("ep", None, None),
        P("ep", None, None),
    )
    return jax.shard_map(
        on_device,
        mesh=mesh,
        in_specs=placed,
        out_specs=(P(("ep", "tp"), None), P(("ep", "tp"), None)),
        check_vma=False,
    )
```

```python
import functools

import jax
import jax.numpy as jnp
from jax import lax
from jax.experimental import pallas as pl
from jax.experimental.pallas import tpu as pltpu
from jax.sharding import PartitionSpec as P

HEAD_DIM = 64
WINDOW = 128
SEQS = 1


EPSILON = 1e-05
NEGATIVE = -1e30


def passed_along(value, axis, steps):
    count = lax.axis_size(axis)
    first, last = (max(0, -steps), min(count, count - steps))
    return lax.ppermute(value, axis, [(source, source + steps) for source in range(first, last)])


def clamped_unit(gate_pre, up_pre):
    gate_cut = jnp.minimum(gate_pre, 7.0)
    up_cut = jnp.clip(up_pre, -7.0, 7.0)
    return gate_cut * jax.nn.sigmoid(1.702 * gate_cut) * (up_cut + 1.0)


def attend(queries, head_keys, head_values, sink_logits, out_weight):
    tok_rows = queries.shape[0]
    local_heads = sink_logits.shape[0]
    local_kv = head_keys.shape[1] // HEAD_DIM
    per_group = local_heads // local_kv
    block_count = tok_rows // WINDOW
    key_width = local_kv * HEAD_DIM
    kv_rows = jnp.concatenate([head_keys, head_values], axis=1)
    earlier = passed_along(kv_rows[tok_rows - WINDOW :], "ep", 1)
    extended = jnp.concatenate([earlier, kv_rows], axis=0)
    banded = jnp.concatenate(
        [
            extended[:tok_rows].reshape(block_count, WINDOW, 2 * key_width),
            kv_rows.reshape(block_count, WINDOW, 2 * key_width),
        ],
        axis=1,
    )
    band_keys = banded[:, :, :key_width].reshape(block_count, 2 * WINDOW, local_kv, HEAD_DIM)
    band_values = banded[:, :, key_width:].reshape(block_count, 2 * WINDOW, local_kv, HEAD_DIM)
    blocked = queries.reshape(block_count, WINDOW, local_kv, per_group, HEAD_DIM)
    scores = jnp.einsum(
        "nqkgd,nskd->nkgqs", blocked, band_keys, preferred_element_type=jnp.float32
    ) * HEAD_DIM ** (-0.5)
    offset = lax.axis_index("ep") * tok_rows
    seq_len = tok_rows * lax.axis_size("ep") // SEQS
    query_pos = offset + jnp.arange(tok_rows, dtype=jnp.int32).reshape(block_count, WINDOW)
    key_pos = (
        offset
        - WINDOW
        + (jnp.arange(block_count, dtype=jnp.int32) * WINDOW)[:, None]
        + jnp.arange(2 * WINDOW, dtype=jnp.int32)[None, :]
    )
    distance = query_pos[:, :, None] - key_pos[:, None, :]
    starts = query_pos // seq_len * seq_len
    valid = (distance >= 0) & (distance < WINDOW) & (key_pos[:, None, :] >= starts[:, :, None])
    scores = jnp.where(valid[:, None, None], scores, NEGATIVE)
    sinks = sink_logits.reshape(local_kv, per_group, 1, 1)
    maxima = jnp.maximum(jnp.max(scores, axis=-1, keepdims=True), sinks)
    powers = jnp.exp(scores - maxima)
    weights = (powers / (jnp.sum(powers, axis=-1, keepdims=True) + jnp.exp(sinks - maxima))).astype(
        jnp.bfloat16
    )
    heads_out = jnp.einsum(
        "nkgqs,nskd->nqkgd", weights, band_values, preferred_element_type=jnp.float32
    )
    heads_out = heads_out.astype(jnp.bfloat16).reshape(tok_rows, local_heads * HEAD_DIM)
    summed = lax.psum_scatter(
        jnp.dot(heads_out, out_weight, preferred_element_type=jnp.float32),
        "tp",
        scatter_dimension=0,
        tiled=True,
    )
    return summed.astype(jnp.bfloat16)


def experts_part(moe_input, norm_gain, routes, route_weight, gate_weight, up_weight, down_weight):
    tok_rows, model_width = moe_input.shape
    choice_count = routes.shape[1]
    targets = lax.axis_size("ep")
    capacity = 2 * choice_count * tok_rows // targets
    values32 = moe_input.astype(jnp.float32)
    scale = lax.rsqrt(jnp.mean(values32 * values32, axis=-1, keepdims=True) + EPSILON)
    normed = (values32 * scale * norm_gain).astype(jnp.bfloat16)
    if capacity >= tok_rows and targets % ROW == 0 and targets >= 2 * ROW:
        experts = jnp.arange(targets, dtype=jnp.int32)
        named = routes[:, None, :] == experts[None, :, None]
        shares = jnp.sum(jnp.where(named, route_weight[:, None, :], 0.0), axis=2).T
        return fused_experts(normed, shares, gate_weight[0], up_weight[0], down_weight[0])
    if capacity >= tok_rows:
        experts = jnp.arange(targets, dtype=jnp.int32)
        named = routes[:, :, None] == experts[None, None, :]
        shares = jnp.sum(jnp.where(named, route_weight[:, :, None], 0.0), axis=1)
        everyone = lax.all_gather(normed, "ep", axis=0, tiled=True)
        mine = lax.all_to_all(shares.T[:, None], "ep", split_axis=0, concat_axis=0, tiled=True)
        gate_pre = jnp.dot(everyone, gate_weight[0], preferred_element_type=jnp.float32)
        up_pre = jnp.dot(everyone, up_weight[0], preferred_element_type=jnp.float32)
        act = clamped_unit(gate_pre, up_pre).astype(jnp.bfloat16)
        result = jnp.dot(act, down_weight[0], preferred_element_type=jnp.float32)
        part = result.astype(jnp.bfloat16).astype(jnp.float32) * mine.reshape(-1, 1)
        return lax.psum_scatter(
            part.astype(jnp.bfloat16), "ep", scatter_dimension=0, tiled=True
        )
    flat_routes = routes.reshape(-1)
    onehot = (flat_routes[:, None] == jnp.arange(targets, dtype=jnp.int32)[None, :]).astype(
        jnp.int32
    )
    earlier_count = jnp.sum((jnp.cumsum(onehot, axis=0) - onehot) * onehot, axis=1)
    slot_index = flat_routes * capacity + earlier_count
    copies = jnp.repeat(normed, choice_count, axis=0)
    outgoing = jnp.zeros((targets * capacity, model_width), jnp.bfloat16).at[slot_index].set(copies)
    outgoing = outgoing.reshape(targets, capacity, model_width)
    arrived = lax.all_to_all(outgoing, "ep", split_axis=0, concat_axis=0, tiled=True)
    flat_rows = arrived.reshape(-1, model_width)
    gate_pre = jnp.dot(flat_rows, gate_weight[0], preferred_element_type=jnp.float32)
    up_pre = jnp.dot(flat_rows, up_weight[0], preferred_element_type=jnp.float32)
    act = clamped_unit(gate_pre, up_pre).astype(jnp.bfloat16)
    result = jnp.dot(act, down_weight[0], preferred_element_type=jnp.float32).astype(jnp.bfloat16)
    came_back = lax.all_to_all(
        result.reshape(arrived.shape), "ep", split_axis=0, concat_axis=0, tiled=True
    )
    picked = came_back.reshape(targets * capacity, model_width)[slot_index]
    weighted = (
        picked.astype(jnp.float32).reshape(tok_rows, choice_count, model_width)
        * route_weight[:, :, None]
    )
    return jnp.sum(weighted, axis=1).astype(jnp.bfloat16)


ROW = 2
PIECES = 2


def experts_kernel(
    count, rows_hbm, shares_hbm, gate_hbm, up_hbm, down_hbm, out_ref,
    gath, shares, gate_w, up_w, down_w, parts, from_row, onward, from_line,
    local_sem, share_send, share_recv, got, sent_up, sent_down, sent_row,
    row_send, row_recv, line_send, line_recv,
):
    lines = count // ROW
    me = lax.axis_index("ep")
    z, y = me // ROW, me % ROW
    tok_rows = out_ref.shape[0]
    piece = tok_rows // PIECES
    loads = [
        pltpu.make_async_copy(rows_hbm, gath.at[me], local_sem.at[0]),
        pltpu.make_async_copy(shares_hbm, shares.at[me], local_sem.at[1]),
        pltpu.make_async_copy(gate_hbm, gate_w, local_sem.at[2]),
        pltpu.make_async_copy(up_hbm, up_w, local_sem.at[3]),
        pltpu.make_async_copy(down_hbm, down_w, local_sem.at[4]),
    ]
    for load in loads:
        load.start()

    barrier = pltpu.get_barrier_semaphore()
    for step in range(1, count):
        other = lax.rem(me + step, count)
        pl.semaphore_signal(
            barrier, inc=1, device_id={"ep": other}, device_id_type=pl.DeviceIdType.MESH
        )
    pl.semaphore_wait(barrier, count - 1)

    def remote(source, target, send, recv, device):
        return pltpu.make_async_remote_copy(
            src_ref=source,
            dst_ref=target,
            send_sem=send,
            recv_sem=recv,
            device_id={"ep": device},
            device_id_type=pl.DeviceIdType.MESH,
        )

    def share_copy(slot, recv_slot, device):
        return remote(
            shares.at[slot], shares.at[slot], share_send.at[device], share_recv.at[recv_slot], device
        )

    def block_copy(block, h, sems, device):
        view = gath.at[block, pl.ds(h * piece, piece)]
        return remote(view, view, sems.at[block, h], got.at[block, h], device)

    across = z * ROW + (1 - y)
    above = jnp.minimum(z + 1, lines - 1) * ROW + y
    below = jnp.maximum(z - 1, 0) * ROW + y

    loads[0].wait()
    loads[1].wait()
    for h in range(PIECES):
        block_copy(me, h, sent_row, across).start()

        @pl.when(z < lines - 1)
        def _():
            block_copy(me, h, sent_up, above).start()

        @pl.when(z > 0)
        def _():
            block_copy(me, h, sent_down, below).start()

    for step in range(1, count):
        share_copy(me, me, lax.rem(me + step, count)).start()
    for step in range(1, count):
        source = lax.rem(me + step, count)
        remote(
            shares.at[source], shares.at[source], share_send.at[source],
            share_recv.at[source], source,
        ).wait_recv()
    loads[2].wait()
    loads[3].wait()
    loads[4].wait()

    square = (tok_rows, tok_rows)
    eye = lax.broadcasted_iota(jnp.int32, square, 0) == lax.broadcasted_iota(jnp.int32, square, 1)

    def visit(turn, carry):
        distance = turn // 4
        foreign = (turn // 2) % 2
        downward = turn % 2
        line = jnp.where(downward == 1, z + distance, z - distance)
        valid = (line >= 0) & (line < lines) & ((distance > 0) | (downward == 0))
        held = jnp.clip(line, 0, lines - 1) * ROW + jnp.where(foreign == 1, 1 - y, y)

        @pl.when(valid)
        def _():
            for h in range(PIECES):

                @pl.when(held != me)
                def _():
                    block_copy(held, h, sent_row, across).wait_recv()

                @pl.when((foreign == 0) & (distance > 0))
                def _():
                    block_copy(held, h, sent_row, across).start()

                    @pl.when((downward == 0) & (z < lines - 1))
                    def _():
                        block_copy(held, h, sent_up, above).start()

                    @pl.when((downward == 1) & (z > 0))
                    def _():
                        block_copy(held, h, sent_down, below).start()

            rows = gath[held]
            gate_pre = jnp.dot(rows, gate_w[...], preferred_element_type=jnp.float32)
            up_pre = jnp.dot(rows, up_w[...], preferred_element_type=jnp.float32)
            act = clamped_unit(gate_pre, up_pre).astype(jnp.bfloat16)
            share = shares[held, pl.ds(me, 1), :]
            column = jnp.sum(jnp.where(eye, share, 0.0), axis=1, keepdims=True)
            result = jnp.dot(act, down_w[...], preferred_element_type=jnp.float32)
            weighted = result.astype(jnp.bfloat16).astype(jnp.float32) * column
            parts[held] = weighted.astype(jnp.bfloat16)

        return carry

    lax.fori_loop(0, 4 * lines, visit, 0)

    def row_copy(line, h):
        return remote(
            parts.at[line * ROW + (1 - y), pl.ds(h * piece, piece)],
            from_row.at[line, pl.ds(h * piece, piece)],
            row_send.at[line, h],
            row_recv.at[line, h],
            across,
        )

    def line_copy(line, h, downward, device):
        return remote(
            onward.at[line, pl.ds(h * piece, piece)],
            from_line.at[downward, line, pl.ds(h * piece, piece)],
            line_send.at[line, h],
            line_recv.at[downward, line, h],
            device,
        )

    def far_first(turn):
        distance = lines - 1 - turn // 2
        downward = turn % 2
        line = jnp.where(downward == 1, z - distance, z + distance)
        valid = (line >= 0) & (line < lines)
        return distance, downward, valid, jnp.clip(line, 0, lines - 1)

    def send_across(turn, carry):
        distance, downward, valid, line = far_first(turn)

        @pl.when(valid & ((distance > 0) | (downward == 0)))
        def _():
            for h in range(PIECES):
                row_copy(line, h).start()

        return carry

    lax.fori_loop(0, 2 * lines, send_across, 0)

    def pass_on(turn, carry):
        distance, downward, valid, line = far_first(turn)

        @pl.when(valid)
        def _():
            for h in range(PIECES):
                span = pl.ds(h * piece, piece)
                row_copy(line, h).wait_recv()
                base = parts[line * ROW + y, span].astype(jnp.float32) + from_row[
                    line, span
                ].astype(jnp.float32)

                @pl.when(downward == 0)
                def _():
                    @pl.when(z > 0)
                    def _():
                        line_copy(line, h, 0, above).wait_recv()
                        onward[line, span] = (
                            base + from_line[0, line, span].astype(jnp.float32)
                        ).astype(jnp.bfloat16)

                    @pl.when(z == 0)
                    def _():
                        onward[line, span] = base.astype(jnp.bfloat16)

                    line_copy(line, h, 0, above).start()

                @pl.when(downward == 1)
                def _():
                    @pl.when(z < lines - 1)
                    def _():
                        line_copy(line, h, 1, below).wait_recv()
                        onward[line, span] = (
                            base + from_line[1, line, span].astype(jnp.float32)
                        ).astype(jnp.bfloat16)

                    @pl.when(z == lines - 1)
                    def _():
                        onward[line, span] = base.astype(jnp.bfloat16)

                    line_copy(line, h, 1, below).start()

        return carry

    lax.fori_loop(0, 2 * (lines - 1), pass_on, 0)

    for h in range(PIECES):
        span = pl.ds(h * piece, piece)
        place = slice(h * piece, (h + 1) * piece)
        row_copy(z, h).wait_recv()
        base = parts[me, span].astype(jnp.float32) + from_row[z, span].astype(jnp.float32)

        @pl.when(z > 0)
        def _():
            line_copy(z, h, 0, above).wait_recv()

        @pl.when(z < lines - 1)
        def _():
            line_copy(z, h, 1, below).wait_recv()

        @pl.when(z == 0)
        def _():
            total = base + from_line[1, z, span].astype(jnp.float32)
            out_ref[place] = total.astype(jnp.bfloat16)

        @pl.when(z == lines - 1)
        def _():
            total = base + from_line[0, z, span].astype(jnp.float32)
            out_ref[place] = total.astype(jnp.bfloat16)

        @pl.when((z > 0) & (z < lines - 1))
        def _():
            total = base + (
                from_line[0, z, span].astype(jnp.float32)
                + from_line[1, z, span].astype(jnp.float32)
            )
            out_ref[place] = total.astype(jnp.bfloat16)

    for step in range(1, count):
        share_copy(me, me, lax.rem(me + step, count)).wait_send()

    def finish(line, carry):
        held = line * ROW + y
        for h in range(PIECES):
            block_copy(held, h, sent_row, across).wait_send()
            row_copy(line, h).wait_send()

            @pl.when((line <= z) & (z < lines - 1))
            def _():
                block_copy(held, h, sent_up, above).wait_send()

            @pl.when((line >= z) & (z > 0))
            def _():
                block_copy(held, h, sent_down, below).wait_send()

            @pl.when(line != z)
            def _():
                line_copy(line, h, 0, above).wait_send()

        return carry

    lax.fori_loop(0, lines, finish, 0)


def fused_experts(normed, shares, gate_weight, up_weight, down_weight):
    count = lax.axis_size("ep")
    lines = count // ROW
    tok_rows, width = normed.shape
    hidden = gate_weight.shape[1]
    block = (tok_rows, width)
    sem = pltpu.SemaphoreType.DMA
    flops = 6 * count * tok_rows * width * hidden
    return pl.pallas_call(
        functools.partial(experts_kernel, count),
        out_shape=jax.ShapeDtypeStruct(block, jnp.bfloat16),
        in_specs=[pl.BlockSpec(memory_space=pl.ANY)] * 5,
        out_specs=pl.BlockSpec(memory_space=pltpu.VMEM),
        scratch_shapes=[
            pltpu.VMEM((count,) + block, jnp.bfloat16),
            pltpu.VMEM((count, count, tok_rows), jnp.float32),
            pltpu.VMEM((width, hidden), jnp.bfloat16),
            pltpu.VMEM((width, hidden), jnp.bfloat16),
            pltpu.VMEM((hidden, width), jnp.bfloat16),
            pltpu.VMEM((count,) + block, jnp.bfloat16),
            pltpu.VMEM((lines,) + block, jnp.bfloat16),
            pltpu.VMEM((lines,) + block, jnp.bfloat16),
            pltpu.VMEM((2, lines) + block, jnp.bfloat16),
            sem((5,)),
            sem((count,)),
            sem((count,)),
            sem((count, PIECES)),
            sem((count, PIECES)),
            sem((count, PIECES)),
            sem((count, PIECES)),
            sem((lines, PIECES)),
            sem((lines, PIECES)),
            sem((lines, PIECES)),
            sem((2, lines, PIECES)),
        ],
        compiler_params=pltpu.CompilerParams(
            collective_id=0, has_side_effects=True, vmem_limit_bytes=44 * 1024 * 1024
        ),
        cost_estimate=pl.CostEstimate(
            flops=10 * flops, bytes_accessed=count * tok_rows * width * 8, transcendentals=0
        ),
    )(normed, shares, gate_weight, up_weight, down_weight)


def on_device(
    queries,
    head_keys,
    head_values,
    sink_logits,
    out_weight,
    moe_input,
    norm_gain,
    routes,
    route_weight,
    gate_weight,
    up_weight,
    down_weight,
):
    attention_out = attend(queries, head_keys, head_values, sink_logits, out_weight)
    routed_out = experts_part(
        moe_input, norm_gain, routes, route_weight, gate_weight, up_weight, down_weight
    )
    return (attention_out, routed_out)


def solution(mesh):
    placed = (
        P("ep", "tp"),
        P("ep", "tp"),
        P("ep", "tp"),
        P("tp"),
        P("tp", None),
        P(("ep", "tp"), None),
        P(),
        P(("ep", "tp"), None),
        P(("ep", "tp"), None),
        P("ep", None, None),
        P("ep", None, None),
        P("ep", None, None),
    )
    return jax.shard_map(
        on_device,
        mesh=mesh,
        in_specs=placed,
        out_specs=(P(("ep", "tp"), None), P(("ep", "tp"), None)),
        check_vma=False,
    )
```

```python
import functools

import jax
import jax.numpy as jnp
from jax import lax
from jax.experimental import pallas as pl
from jax.experimental.pallas import tpu as pltpu
from jax.sharding import PartitionSpec as P

HEAD_DIM = 64
WINDOW = 128
SEQS = 1


EPSILON = 1e-05
NEGATIVE = -1e30


def passed_along(value, axis, steps):
    count = lax.axis_size(axis)
    first, last = (max(0, -steps), min(count, count - steps))
    return lax.ppermute(value, axis, [(source, source + steps) for source in range(first, last)])


def clamped_unit(gate_pre, up_pre):
    gate_cut = jnp.minimum(gate_pre, 7.0)
    up_cut = jnp.clip(up_pre, -7.0, 7.0)
    return gate_cut * jax.nn.sigmoid(1.702 * gate_cut) * (up_cut + 1.0)


def attention_kernel(seq_blocks, sinks, q_ref, k_ref, v_ref, edge_ref, weight_ref, out_ref):
    block = pl.program_id(0)
    local_kv = k_ref.shape[1] // HEAD_DIM
    local_heads = q_ref.shape[1] // HEAD_DIM
    per_group = local_heads // local_kv
    key_width = local_kv * HEAD_DIM
    opens = lax.rem(lax.axis_index("ep") * pl.num_programs(0) + block, seq_blocks) == 0
    now = pl.ds(pl.multiple_of(block * WINDOW, WINDOW), WINDOW)
    before = pl.ds(pl.multiple_of(jnp.maximum(block - 1, 0) * WINDOW, WINDOW), WINDOW)
    edge = edge_ref[...]
    keys = jnp.concatenate(
        [jnp.where(block == 0, edge[:, :key_width], k_ref[before, :]), k_ref[now, :]], axis=0
    )
    values = jnp.concatenate(
        [jnp.where(block == 0, edge[:, key_width:], v_ref[before, :]), v_ref[now, :]], axis=0
    )
    shape = (WINDOW, 2 * WINDOW)
    column = lax.broadcasted_iota(jnp.int32, shape, 1)
    distance = lax.broadcasted_iota(jnp.int32, shape, 0) + WINDOW - column
    lowest = jnp.where(opens, WINDOW, 0)
    valid = (distance >= 0) & (distance < WINDOW) & (column >= lowest)
    outs = []
    for head in range(local_heads):
        group = head // per_group
        span = slice(group * HEAD_DIM, (group + 1) * HEAD_DIM)
        scores = lax.dot_general(
            q_ref[:, head * HEAD_DIM : (head + 1) * HEAD_DIM],
            keys[:, span],
            (((1,), (1,)), ((), ())),
            preferred_element_type=jnp.float32,
        ) * HEAD_DIM ** (-0.5)
        scores = jnp.where(valid, scores, NEGATIVE)
        sink = sinks[head]
        maxima = jnp.maximum(jnp.max(scores, axis=-1, keepdims=True), sink)
        powers = jnp.exp(scores - maxima)
        total = jnp.sum(powers, axis=-1, keepdims=True) + jnp.exp(sink - maxima)
        weights = (powers / total).astype(jnp.bfloat16)
        outs.append(jnp.dot(weights, values[:, span], preferred_element_type=jnp.float32))
    heads_out = jnp.concatenate(outs, axis=1).astype(jnp.bfloat16)
    out_ref[...] = jnp.dot(heads_out, weight_ref[...], preferred_element_type=jnp.float32)


def attend(queries, head_keys, head_values, sink_logits, out_weight):
    tok_rows, width = queries.shape
    seq_len = tok_rows * lax.axis_size("ep") // SEQS
    last = tok_rows - WINDOW
    edge = passed_along(
        jnp.concatenate([head_keys[last:], head_values[last:]], axis=1), "ep", 1
    )
    columns = out_weight.shape[1]
    whole = lambda array: pl.BlockSpec(array.shape, lambda block: (0, 0))
    partial = pl.pallas_call(
        functools.partial(attention_kernel, seq_len // WINDOW),
        grid=(tok_rows // WINDOW,),
        out_shape=jax.ShapeDtypeStruct((tok_rows, columns), jnp.float32),
        in_specs=[
            pl.BlockSpec(memory_space=pltpu.SMEM),
            pl.BlockSpec((WINDOW, width), lambda block: (block, 0)),
            whole(head_keys),
            whole(head_values),
            whole(edge),
            whole(out_weight),
        ],
        out_specs=pl.BlockSpec((WINDOW, columns), lambda block: (block, 0)),
        cost_estimate=pl.CostEstimate(
            flops=4 * tok_rows * width * columns,
            bytes_accessed=4 * tok_rows * columns,
            transcendentals=0,
        ),
    )(sink_logits, queries, head_keys, head_values, edge, out_weight)
    summed = lax.psum_scatter(partial, "tp", scatter_dimension=0, tiled=True)
    return summed.astype(jnp.bfloat16)


def experts_part(moe_input, norm_gain, routes, route_weight, gate_weight, up_weight, down_weight):
    tok_rows, model_width = moe_input.shape
    choice_count = routes.shape[1]
    targets = lax.axis_size("ep")
    capacity = 2 * choice_count * tok_rows // targets
    values32 = moe_input.astype(jnp.float32)
    scale = lax.rsqrt(jnp.mean(values32 * values32, axis=-1, keepdims=True) + EPSILON)
    normed = (values32 * scale * norm_gain).astype(jnp.bfloat16)
    if capacity >= tok_rows and targets % ROW == 0 and targets >= 2 * ROW:
        experts = jnp.arange(targets, dtype=jnp.int32)
        named = routes[:, None, :] == experts[None, :, None]
        shares = jnp.sum(jnp.where(named, route_weight[:, None, :], 0.0), axis=2).T
        return fused_experts(normed, shares, gate_weight[0], up_weight[0], down_weight[0])
    if capacity >= tok_rows:
        experts = jnp.arange(targets, dtype=jnp.int32)
        named = routes[:, :, None] == experts[None, None, :]
        shares = jnp.sum(jnp.where(named, route_weight[:, :, None], 0.0), axis=1)
        everyone = lax.all_gather(normed, "ep", axis=0, tiled=True)
        mine = lax.all_to_all(shares.T[:, None], "ep", split_axis=0, concat_axis=0, tiled=True)
        gate_pre = jnp.dot(everyone, gate_weight[0], preferred_element_type=jnp.float32)
        up_pre = jnp.dot(everyone, up_weight[0], preferred_element_type=jnp.float32)
        act = clamped_unit(gate_pre, up_pre).astype(jnp.bfloat16)
        result = jnp.dot(act, down_weight[0], preferred_element_type=jnp.float32)
        part = result.astype(jnp.bfloat16).astype(jnp.float32) * mine.reshape(-1, 1)
        return lax.psum_scatter(
            part.astype(jnp.bfloat16), "ep", scatter_dimension=0, tiled=True
        )
    flat_routes = routes.reshape(-1)
    onehot = (flat_routes[:, None] == jnp.arange(targets, dtype=jnp.int32)[None, :]).astype(
        jnp.int32
    )
    earlier_count = jnp.sum((jnp.cumsum(onehot, axis=0) - onehot) * onehot, axis=1)
    slot_index = flat_routes * capacity + earlier_count
    copies = jnp.repeat(normed, choice_count, axis=0)
    outgoing = jnp.zeros((targets * capacity, model_width), jnp.bfloat16).at[slot_index].set(copies)
    outgoing = outgoing.reshape(targets, capacity, model_width)
    arrived = lax.all_to_all(outgoing, "ep", split_axis=0, concat_axis=0, tiled=True)
    flat_rows = arrived.reshape(-1, model_width)
    gate_pre = jnp.dot(flat_rows, gate_weight[0], preferred_element_type=jnp.float32)
    up_pre = jnp.dot(flat_rows, up_weight[0], preferred_element_type=jnp.float32)
    act = clamped_unit(gate_pre, up_pre).astype(jnp.bfloat16)
    result = jnp.dot(act, down_weight[0], preferred_element_type=jnp.float32).astype(jnp.bfloat16)
    came_back = lax.all_to_all(
        result.reshape(arrived.shape), "ep", split_axis=0, concat_axis=0, tiled=True
    )
    picked = came_back.reshape(targets * capacity, model_width)[slot_index]
    weighted = (
        picked.astype(jnp.float32).reshape(tok_rows, choice_count, model_width)
        * route_weight[:, :, None]
    )
    return jnp.sum(weighted, axis=1).astype(jnp.bfloat16)


ROW = 2
PIECES = 2


def experts_kernel(
    count, rows_hbm, shares_hbm, gate_hbm, up_hbm, down_hbm, out_ref,
    gath, shares, gate_w, up_w, down_w, parts, from_row, onward, from_line,
    local_sem, share_send, share_recv, got, sent_up, sent_down, sent_row,
    row_send, row_recv, line_send, line_recv,
):
    lines = count // ROW
    me = lax.axis_index("ep")
    z, y = me // ROW, me % ROW
    tok_rows = out_ref.shape[0]
    piece = tok_rows // PIECES
    loads = [
        pltpu.make_async_copy(rows_hbm, gath.at[me], local_sem.at[0]),
        pltpu.make_async_copy(shares_hbm, shares.at[me], local_sem.at[1]),
        pltpu.make_async_copy(gate_hbm, gate_w, local_sem.at[2]),
        pltpu.make_async_copy(up_hbm, up_w, local_sem.at[3]),
        pltpu.make_async_copy(down_hbm, down_w, local_sem.at[4]),
    ]
    for load in loads:
        load.start()

    barrier = pltpu.get_barrier_semaphore()
    for step in range(1, count):
        other = lax.rem(me + step, count)
        pl.semaphore_signal(
            barrier, inc=1, device_id={"ep": other}, device_id_type=pl.DeviceIdType.MESH
        )
    pl.semaphore_wait(barrier, count - 1)

    def remote(source, target, send, recv, device):
        return pltpu.make_async_remote_copy(
            src_ref=source,
            dst_ref=target,
            send_sem=send,
            recv_sem=recv,
            device_id={"ep": device},
            device_id_type=pl.DeviceIdType.MESH,
        )

    def share_copy(slot, recv_slot, device):
        return remote(
            shares.at[slot], shares.at[slot], share_send.at[device], share_recv.at[recv_slot], device
        )

    def block_copy(block, h, sems, device):
        view = gath.at[block, pl.ds(h * piece, piece)]
        return remote(view, view, sems.at[block, h], got.at[block, h], device)

    across = z * ROW + (1 - y)
    above = jnp.minimum(z + 1, lines - 1) * ROW + y
    below = jnp.maximum(z - 1, 0) * ROW + y

    loads[0].wait()
    loads[1].wait()
    for h in range(PIECES):
        block_copy(me, h, sent_row, across).start()

        @pl.when(z < lines - 1)
        def _():
            block_copy(me, h, sent_up, above).start()

        @pl.when(z > 0)
        def _():
            block_copy(me, h, sent_down, below).start()

    for step in range(1, count):
        share_copy(me, me, lax.rem(me + step, count)).start()
    for step in range(1, count):
        source = lax.rem(me + step, count)
        remote(
            shares.at[source], shares.at[source], share_send.at[source],
            share_recv.at[source], source,
        ).wait_recv()
    loads[2].wait()
    loads[3].wait()
    loads[4].wait()

    square = (tok_rows, tok_rows)
    eye = lax.broadcasted_iota(jnp.int32, square, 0) == lax.broadcasted_iota(jnp.int32, square, 1)

    def visit(turn, carry):
        distance = turn // 4
        foreign = (turn // 2) % 2
        downward = turn % 2
        line = jnp.where(downward == 1, z + distance, z - distance)
        valid = (line >= 0) & (line < lines) & ((distance > 0) | (downward == 0))
        held = jnp.clip(line, 0, lines - 1) * ROW + jnp.where(foreign == 1, 1 - y, y)

        @pl.when(valid)
        def _():
            for h in range(PIECES):

                @pl.when(held != me)
                def _():
                    block_copy(held, h, sent_row, across).wait_recv()

                @pl.when((foreign == 0) & (distance > 0))
                def _():
                    block_copy(held, h, sent_row, across).start()

                    @pl.when((downward == 0) & (z < lines - 1))
                    def _():
                        block_copy(held, h, sent_up, above).start()

                    @pl.when((downward == 1) & (z > 0))
                    def _():
                        block_copy(held, h, sent_down, below).start()

            rows = gath[held]
            gate_pre = jnp.dot(rows, gate_w[...], preferred_element_type=jnp.float32)
            up_pre = jnp.dot(rows, up_w[...], preferred_element_type=jnp.float32)
            act = clamped_unit(gate_pre, up_pre).astype(jnp.bfloat16)
            share = shares[held, pl.ds(me, 1), :]
            column = jnp.sum(jnp.where(eye, share, 0.0), axis=1, keepdims=True)
            result = jnp.dot(act, down_w[...], preferred_element_type=jnp.float32)
            weighted = result.astype(jnp.bfloat16).astype(jnp.float32) * column
            parts[held] = weighted.astype(jnp.bfloat16)

        return carry

    lax.fori_loop(0, 4 * lines, visit, 0)

    def row_copy(line, h):
        return remote(
            parts.at[line * ROW + (1 - y), pl.ds(h * piece, piece)],
            from_row.at[line, pl.ds(h * piece, piece)],
            row_send.at[line, h],
            row_recv.at[line, h],
            across,
        )

    def line_copy(line, h, downward, device):
        return remote(
            onward.at[line, pl.ds(h * piece, piece)],
            from_line.at[downward, line, pl.ds(h * piece, piece)],
            line_send.at[line, h],
            line_recv.at[downward, line, h],
            device,
        )

    def far_first(turn):
        distance = lines - 1 - turn // 2
        downward = turn % 2
        line = jnp.where(downward == 1, z - distance, z + distance)
        valid = (line >= 0) & (line < lines)
        return distance, downward, valid, jnp.clip(line, 0, lines - 1)

    def send_across(turn, carry):
        distance, downward, valid, line = far_first(turn)

        @pl.when(valid & ((distance > 0) | (downward == 0)))
        def _():
            for h in range(PIECES):
                row_copy(line, h).start()

        return carry

    lax.fori_loop(0, 2 * lines, send_across, 0)

    def pass_on(turn, carry):
        distance, downward, valid, line = far_first(turn)

        @pl.when(valid)
        def _():
            for h in range(PIECES):
                span = pl.ds(h * piece, piece)
                row_copy(line, h).wait_recv()
                base = parts[line * ROW + y, span].astype(jnp.float32) + from_row[
                    line, span
                ].astype(jnp.float32)

                @pl.when(downward == 0)
                def _():
                    @pl.when(z > 0)
                    def _():
                        line_copy(line, h, 0, above).wait_recv()
                        onward[line, span] = (
                            base + from_line[0, line, span].astype(jnp.float32)
                        ).astype(jnp.bfloat16)

                    @pl.when(z == 0)
                    def _():
                        onward[line, span] = base.astype(jnp.bfloat16)

                    line_copy(line, h, 0, above).start()

                @pl.when(downward == 1)
                def _():
                    @pl.when(z < lines - 1)
                    def _():
                        line_copy(line, h, 1, below).wait_recv()
                        onward[line, span] = (
                            base + from_line[1, line, span].astype(jnp.float32)
                        ).astype(jnp.bfloat16)

                    @pl.when(z == lines - 1)
                    def _():
                        onward[line, span] = base.astype(jnp.bfloat16)

                    line_copy(line, h, 1, below).start()

        return carry

    lax.fori_loop(0, 2 * (lines - 1), pass_on, 0)

    for h in range(PIECES):
        span = pl.ds(h * piece, piece)
        place = slice(h * piece, (h + 1) * piece)
        row_copy(z, h).wait_recv()
        base = parts[me, span].astype(jnp.float32) + from_row[z, span].astype(jnp.float32)

        @pl.when(z > 0)
        def _():
            line_copy(z, h, 0, above).wait_recv()

        @pl.when(z < lines - 1)
        def _():
            line_copy(z, h, 1, below).wait_recv()

        @pl.when(z == 0)
        def _():
            total = base + from_line[1, z, span].astype(jnp.float32)
            out_ref[place] = total.astype(jnp.bfloat16)

        @pl.when(z == lines - 1)
        def _():
            total = base + from_line[0, z, span].astype(jnp.float32)
            out_ref[place] = total.astype(jnp.bfloat16)

        @pl.when((z > 0) & (z < lines - 1))
        def _():
            total = base + (
                from_line[0, z, span].astype(jnp.float32)
                + from_line[1, z, span].astype(jnp.float32)
            )
            out_ref[place] = total.astype(jnp.bfloat16)

    for step in range(1, count):
        share_copy(me, me, lax.rem(me + step, count)).wait_send()

    def finish(line, carry):
        held = line * ROW + y
        for h in range(PIECES):
            block_copy(held, h, sent_row, across).wait_send()
            row_copy(line, h).wait_send()

            @pl.when((line <= z) & (z < lines - 1))
            def _():
                block_copy(held, h, sent_up, above).wait_send()

            @pl.when((line >= z) & (z > 0))
            def _():
                block_copy(held, h, sent_down, below).wait_send()

            @pl.when(line != z)
            def _():
                line_copy(line, h, 0, above).wait_send()

        return carry

    lax.fori_loop(0, lines, finish, 0)


def fused_experts(normed, shares, gate_weight, up_weight, down_weight):
    count = lax.axis_size("ep")
    lines = count // ROW
    tok_rows, width = normed.shape
    hidden = gate_weight.shape[1]
    block = (tok_rows, width)
    sem = pltpu.SemaphoreType.DMA
    flops = 6 * count * tok_rows * width * hidden
    return pl.pallas_call(
        functools.partial(experts_kernel, count),
        out_shape=jax.ShapeDtypeStruct(block, jnp.bfloat16),
        in_specs=[pl.BlockSpec(memory_space=pl.ANY)] * 5,
        out_specs=pl.BlockSpec(memory_space=pltpu.VMEM),
        scratch_shapes=[
            pltpu.VMEM((count,) + block, jnp.bfloat16),
            pltpu.VMEM((count, count, tok_rows), jnp.float32),
            pltpu.VMEM((width, hidden), jnp.bfloat16),
            pltpu.VMEM((width, hidden), jnp.bfloat16),
            pltpu.VMEM((hidden, width), jnp.bfloat16),
            pltpu.VMEM((count,) + block, jnp.bfloat16),
            pltpu.VMEM((lines,) + block, jnp.bfloat16),
            pltpu.VMEM((lines,) + block, jnp.bfloat16),
            pltpu.VMEM((2, lines) + block, jnp.bfloat16),
            sem((5,)),
            sem((count,)),
            sem((count,)),
            sem((count, PIECES)),
            sem((count, PIECES)),
            sem((count, PIECES)),
            sem((count, PIECES)),
            sem((lines, PIECES)),
            sem((lines, PIECES)),
            sem((lines, PIECES)),
            sem((2, lines, PIECES)),
        ],
        compiler_params=pltpu.CompilerParams(
            collective_id=0, has_side_effects=True, vmem_limit_bytes=44 * 1024 * 1024
        ),
        cost_estimate=pl.CostEstimate(
            flops=10 * flops, bytes_accessed=count * tok_rows * width * 8, transcendentals=0
        ),
    )(normed, shares, gate_weight, up_weight, down_weight)


def on_device(
    queries,
    head_keys,
    head_values,
    sink_logits,
    out_weight,
    moe_input,
    norm_gain,
    routes,
    route_weight,
    gate_weight,
    up_weight,
    down_weight,
):
    attention_out = attend(queries, head_keys, head_values, sink_logits, out_weight)
    routed_out = experts_part(
        moe_input, norm_gain, routes, route_weight, gate_weight, up_weight, down_weight
    )
    return (attention_out, routed_out)


def solution(mesh):
    placed = (
        P("ep", "tp"),
        P("ep", "tp"),
        P("ep", "tp"),
        P("tp"),
        P("tp", None),
        P(("ep", "tp"), None),
        P(),
        P(("ep", "tp"), None),
        P(("ep", "tp"), None),
        P("ep", None, None),
        P("ep", None, None),
        P("ep", None, None),
    )
    return jax.shard_map(
        on_device,
        mesh=mesh,
        in_specs=placed,
        out_specs=(P(("ep", "tp"), None), P(("ep", "tp"), None)),
        check_vma=False,
    )
```
